128 devices in a mesh: ep: 128 (over z, y, x, core).
Axes of the slice: x: 4, y: 4, z: 4, core: 2. Of those that a mesh axis runs over, the one named last changes fastest.
Arguments:
- tokens: bfloat16 [2048, 1024], P('ep'), may hold values from -6 to 6
- lengths: int32 [2048], P('ep'), may hold values from 1 to 8191
- cache_keys: bfloat16 [2048, 128, 512], P('ep'), may hold values from -6 to 6
- cache_values: bfloat16 [2048, 128, 1024], P('ep'), may hold values from -6 to 6
- retention_state: float32 [2048, 4, 128, 256], P('ep'), may hold values from -24 to 24
- mix_gain: float32 [1024], replicated, may hold values from 0.1 to 1.9
- query_weight: bfloat16 [1024, 512], replicated, may hold values from -0.1875 to 0.1875
- key_weight: bfloat16 [1024, 512], replicated, may hold values from -0.1875 to 0.1875
- value_weight: bfloat16 [1024, 1024], replicated, may hold values from -0.1875 to 0.1875
- out_weight: bfloat16 [1024, 1024], replicated, may hold values from -0.1875 to 0.1875
- ffn_gain: float32 [1024], replicated, may hold values from 0.1 to 1.9
- routes: int32 [2048, 6], P('ep'), may hold values from 0 to 127, all different within a row; in each aligned block of 16 rows (0 to 15, 16 to 31, ...) at most 2 rows name the same one
- route_scores: float32 [2048, 6], P('ep'), may hold values from 0.05 to 1
- expert_gate: bfloat16 [128, 1024, 256], P('ep'), may hold values from -0.1875 to 0.1875
- expert_up: bfloat16 [128, 1024, 256], P('ep'), may hold values from -0.1875 to 0.1875
- expert_down: bfloat16 [128, 256, 1024], P('ep'), may hold values from -0.375 to 0.375
- shared_gate: bfloat16 [1024, 256], replicated, may hold values from -0.1875 to 0.1875
- shared_up: bfloat16 [1024, 256], replicated, may hold values from -0.1875 to 0.1875
- shared_down: bfloat16 [256, 1024], replicated, may hold values from -0.375 to 0.375
- dense_gate: bfloat16 [4096, 1024], P('ep'), may hold values from -0.1875 to 0.1875
- dense_up: bfloat16 [4096, 1024], P('ep'), may hold values from -0.1875 to 0.1875
- dense_down: bfloat16 [4096, 1024], P('ep'), may hold values from -0.09375 to 0.09375
- dense_mix: float32 [1024], replicated, may hold values from -3 to 3
Outputs:
- layer_out: bfloat16 [2048, 1024], P('ep')
- new_keys: bfloat16 [2048, 512], P('ep')
- new_values: bfloat16 [2048, 1024], P('ep')
The draws below stay inside these ranges and needn't reach their ends.
Inputs may be any that keep to these rules, and one draw needn't show every extreme that they name: `routes`: each row names 6 different experts; among the rows of one device no expert is named more than 2 times.
All inputs are finite; a program needn't handle non-finite values.
Results may differ from the reference program's by a relative error of at most 0.012.
Values may be sent and summed in bfloat16 or wider, within the bound.
A program may use at most 128 MiB of HBM per device.

```python
import math
import jax
import jax.numpy as jnp
import numpy as np
from jax import lax

D = 1024
HEADS = 4
DK = 128
DV = 256
BLOCK = 128
SEQ_DEV = 16
SEQS = 2048
EXPERTS = 128
TOP_K = 6
CAP = 2
EH = 256
SH = 256
DENSE_FF = 4096
N_EP = 128


def plant(values, stream_key, smallest, top_value):
    dims = values.shape
    spot = [jax.random.randint(jax.random.fold_in(stream_key, axis), (), 0, dims[axis]) for axis in range(len(dims))]
    values = values.at[tuple(spot)].set(smallest)
    longest = dims.index(max(dims))
    spot[longest] = (spot[longest] + 1) % dims[longest]
    return values.at[tuple(spot)].set(top_value)


def shard_levels(rng, dims, shards, low, high):
    factor_of = 1.0
    for axis_at, shards_of in shards:
        heights = jax.random.uniform(jax.random.fold_in(jax.random.fold_in(rng, 6), axis_at), (shards_of,), jnp.float32, low / len(shards), high / len(shards))
        factor_of = factor_of * jnp.repeat(jnp.exp(heights), dims[axis_at] // shards_of).reshape((-1,) + (1,) * (len(dims) - 1 - axis_at))
    return factor_of


def routed_block(key, own, number, rows, count, top, reach, slope):
    sequence = jax.random.permutation(key, count)
    crowded, common = portions_of(count, rows * top, reach, slope, True), portions_of(count, rows * top, reach, slope, False)
    places = jnp.arange(count)

    def named(tallies, offset_by):
        used = int((tallies > 0).sum())
        fixed = max(1, used // 4)
        passed = fixed + (places - fixed + offset_by * (used - fixed)) % max(1, count - fixed)
        return jnp.zeros((count,), jnp.int32).at[sequence[jnp.where(places < fixed, places, passed)]].set(jnp.asarray(tallies, jnp.int32))

    tallies = jnp.where(number % 4 == 0, named(crowded, number // 4), named(common, number - number // 4 - 1))
    mixed = jax.random.permutation(jax.random.fold_in(own, 3), count)
    donor, receiver = mixed[0:count // 2 * 2:2], mixed[1:count // 2 * 2:2]
    room = jnp.minimum(tallies[donor] - 1, reach - tallies[receiver]) // 2
    room = jnp.where((donor == sequence[0]) | (receiver == sequence[0]) | (tallies[receiver] == 0), 0, jnp.maximum(room, 0))
    passed = jax.random.randint(jax.random.fold_in(own, 4), (count // 2,), 0, 1 << 20) % (room + 1)
    tallies = tallies.at[donor].add(-passed).at[receiver].add(passed)
    members = jnp.searchsorted(jnp.cumsum(tallies), jnp.arange(rows * top), side="right").astype(jnp.int32)
    grid = members.reshape(top, rows).T
    grid = grid[jax.random.permutation(jax.random.fold_in(own, 1), rows)]
    offset_by = jax.random.randint(jax.random.fold_in(own, 2), (rows, 1), 0, top)
    return jnp.take_along_axis(grid, (jnp.arange(top)[None, :] + offset_by) % top, axis=1)


def portions_of(amount, total, limit, slope, full):
    portions = [(1 << 20) // math.isqrt(grade ** slope) + 1 for grade in range(1, amount + 1)]
    largest = limit if full else min(limit, max(-(-total // amount), total * portions[0] // sum(portions)))
    least = 1 if total - largest >= amount - 1 else 0
    counts, surplus = [largest] + [least] * (amount - 1), total - largest - least * (amount - 1)
    while surplus > 0:
        free = [i for i in range(1, amount) if counts[i] < largest] or [i for i in range(1, amount) if counts[i] < limit]
        pool, budget = sum([portions[i] for i in free]), surplus
        for i in free:
            addition = min(limit - counts[i], max(1, budget * portions[i] // pool), surplus)
            counts[i] = counts[i] + addition
            surplus = surplus - addition
    return np.array(counts)


def gaussian(own_key, dims, deviation, reach, shards=(), held_as=jnp.bfloat16):
    result = deviation * jax.random.normal(own_key, dims, jnp.float32)
    if shards:
        result = result * shard_levels(own_key, dims, shards, -0.22, 0.18)
    return jnp.clip(result, -reach, reach).astype(held_as)


def setup_inputs(seed: int = 0) -> dict:
    key_of = jax.random.split(jax.random.key(seed), 24)
    tokens = gaussian(key_of[0], (SEQS, D), 1.0, 6.0, ((0, 128),))
    lengths = plant(jax.random.randint(key_of[1], (SEQS,), 1, 8192), jax.random.fold_in(key_of[1], 1), 1, 8191).astype(jnp.int32)
    cache_keys = gaussian(key_of[2], (SEQS, BLOCK, HEADS * DK), 1.0, 6.0, ((0, 128),))
    cache_values = gaussian(key_of[3], (SEQS, BLOCK, HEADS * DV), 1.0, 6.0, ((0, 128),))
    retention_state = gaussian(key_of[4], (SEQS, HEADS, DK, DV), 4.0, 24.0, ((0, 128),), jnp.float32)
    mix_gain = jnp.clip(1.0 + 0.18 * jax.random.normal(key_of[5], (D,), jnp.float32), 0.1, 1.9)
    query_weight = gaussian(key_of[6], (D, HEADS * DK), D ** -0.5, 0.1875)
    key_weight = gaussian(key_of[7], (D, HEADS * DK), D ** -0.5, 0.1875)
    value_weight = gaussian(key_of[8], (D, HEADS * DV), D ** -0.5, 0.1875)
    out_weight = gaussian(key_of[9], (HEADS * DV, D), (HEADS * DV) ** -0.5, 0.1875)
    ffn_gain = jnp.clip(1.0 + 0.18 * jax.random.normal(key_of[10], (D,), jnp.float32), 0.1, 1.9)
    routes_keys = jax.random.split(jax.random.fold_in(key_of[11], 1), SEQS // SEQ_DEV)
    routes_turns = jax.random.permutation(jax.random.fold_in(key_of[11], 3), SEQS // SEQ_DEV)
    routes = jax.vmap(lambda own, number: routed_block(jax.random.fold_in(key_of[11], 2), own, number, SEQ_DEV, EXPERTS, TOP_K, CAP, 1))(routes_keys, routes_turns).reshape((SEQS, TOP_K))
    route_scores = jnp.clip(0.05 + 0.95 * jax.random.uniform(key_of[12], (SEQS, TOP_K), jnp.float32) ** shard_levels(key_of[12], (SEQS, TOP_K), ((0, 128),), -0.2, 0.2), 0.05, 1.0)
    expert_gate = gaussian(key_of[13], (EXPERTS, D, EH), D ** -0.5, 0.1875, ((0, 128),))
    expert_up = gaussian(key_of[14], (EXPERTS, D, EH), D ** -0.5, 0.1875, ((0, 128),))
    expert_down = gaussian(key_of[15], (EXPERTS, EH, D), EH ** -0.5, 0.375, ((0, 128),))
    shared_gate = gaussian(key_of[16], (D, SH), D ** -0.5, 0.1875)
    shared_up = gaussian(key_of[17], (D, SH), D ** -0.5, 0.1875)
    shared_down = gaussian(key_of[18], (SH, D), SH ** -0.5, 0.375)
    dense_gate = gaussian(key_of[19], (DENSE_FF, D), D ** -0.5, 0.1875, ((0, 128),))
    dense_up = gaussian(key_of[20], (DENSE_FF, D), D ** -0.5, 0.1875, ((0, 128),))
    dense_down = gaussian(key_of[21], (DENSE_FF, D), DENSE_FF ** -0.5, 0.09375, ((0, 128),))
    dense_mix = jnp.clip(jax.random.uniform(key_of[22], (D,), jnp.float32, -3.0, 3.0), -3.0, 3.0)
    return {"tokens": tokens, "lengths": lengths, "cache_keys": cache_keys, "cache_values": cache_values, "retention_state": retention_state, "mix_gain": mix_gain, "query_weight": query_weight, "key_weight": key_weight, "value_weight": value_weight, "out_weight": out_weight, "ffn_gain": ffn_gain, "routes": routes, "route_scores": route_scores, "expert_gate": expert_gate, "expert_up": expert_up, "expert_down": expert_down, "shared_gate": shared_gate, "shared_up": shared_up, "shared_down": shared_down, "dense_gate": dense_gate, "dense_up": dense_up, "dense_down": dense_down, "dense_mix": dense_mix}


eps = 1e-06
route_scale = 2.5
rope_base = 10000.0

def normed(values):
    return values * lax.rsqrt(lax.optimization_barrier(jnp.mean(values * values, axis=-1, keepdims=True)) + eps)

def log_decay(head_count):
    return jnp.log1p(-jnp.exp2(-5.0 - jnp.arange(head_count, dtype=jnp.float32)))

def rotate(values, positions):
    half_size = values.shape[-1] // 2
    inverse = rope_base ** (-jnp.arange(half_size, dtype=jnp.float32) / half_size)
    angles = positions.astype(jnp.float32)[:, None, None] * inverse[None, None, :]
    cosine = jnp.cos(angles)
    sine_part = jnp.sin(angles)
    first_half = values[..., :half_size]
    second = values[..., half_size:]
    return jnp.concatenate([first_half * cosine - second * sine_part, first_half * sine_part + second * cosine], axis=-1)

def swiglu(inputs, w_gate, w_up, w_down):
    gate_part = jnp.dot(inputs, w_gate, preferred_element_type=jnp.float32)
    up_part = jnp.dot(inputs, w_up, preferred_element_type=jnp.float32)
    hidden = (jax.nn.silu(gate_part) * up_part).astype(jnp.bfloat16)
    return jnp.dot(hidden, w_down, preferred_element_type=jnp.float32)

def retain(tokens, lengths, mix_gain, w_query, w_key, w_value, w_out, cache_keys, cache_values, carry_state):
    seq_count, head_count, key_size, value_size = carry_state.shape
    block_size = cache_keys.shape[1]
    widened = tokens.astype(jnp.float32)
    normal_in = (normed(widened) * mix_gain).astype(jnp.bfloat16)
    raw_query = jnp.dot(normal_in, w_query, preferred_element_type=jnp.float32).reshape(seq_count, head_count, key_size)
    raw_key = jnp.dot(normal_in, w_key, preferred_element_type=jnp.float32).reshape(seq_count, head_count, key_size)
    raw_value = jnp.dot(normal_in, w_value, preferred_element_type=jnp.float32).reshape(seq_count, head_count, value_size)
    queries = (rotate(raw_query, lengths) * key_size ** (-0.5)).astype(jnp.bfloat16)
    new_keys = rotate(raw_key, lengths).astype(jnp.bfloat16)
    new_values = raw_value.astype(jnp.bfloat16)
    filled = lengths % block_size
    decay_rate = log_decay(head_count)
    places = jnp.arange(block_size, dtype=jnp.int32)
    stored_keys = cache_keys.reshape(seq_count, block_size, head_count, key_size)
    stored_values = cache_values.reshape(seq_count, block_size, head_count, value_size)
    scores = jnp.einsum('shd,sjhd->shj', queries.astype(jnp.float32), stored_keys.astype(jnp.float32))
    distance = jnp.maximum(filled[:, None] - places[None, :], 0).astype(jnp.float32)
    live_mask = places[None, :] < filled[:, None]
    weighted = jnp.where(live_mask[:, None, :], scores * jnp.exp(distance[:, None, :] * decay_rate[None, :, None]), 0.0).astype(jnp.bfloat16)
    own_weight = lax.optimization_barrier(jnp.sum(queries.astype(jnp.float32) * new_keys.astype(jnp.float32), axis=-1)).astype(jnp.bfloat16)
    inside = jnp.einsum('shj,sjhe->she', weighted.astype(jnp.float32), stored_values.astype(jnp.float32))
    inside = inside + own_weight.astype(jnp.float32)[:, :, None] * new_values.astype(jnp.float32)
    carried = jnp.einsum('shd,shde->she', queries.astype(jnp.float32), carry_state, precision=lax.Precision.HIGHEST)
    carried = carried * jnp.exp((filled.astype(jnp.float32)[:, None] + 1.0) * decay_rate[None, :])[:, :, None]
    headed = normed(inside + carried).astype(jnp.bfloat16).reshape(seq_count, head_count * value_size)
    mixer_out = jnp.dot(headed, w_out, preferred_element_type=jnp.float32)
    residual = widened + normed(mixer_out)
    return (residual, new_keys.reshape(seq_count, head_count * key_size), new_values.reshape(seq_count, head_count * value_size))

def reference(tokens, lengths, cache_keys, cache_values, retention_state, mix_gain, query_weight, key_weight, value_weight, out_weight, ffn_gain, routes, route_scores, expert_gate, expert_up, expert_down, shared_gate, shared_up, shared_down, dense_gate, dense_up, dense_down, dense_mix):
    residual, new_keys, new_values = retain(tokens, lengths, mix_gain, query_weight, key_weight, value_weight, out_weight, cache_keys, cache_values, retention_state)
    normal_ffn = (normed(residual) * ffn_gain).astype(jnp.bfloat16)
    shared_out = swiglu(normal_ffn, shared_gate, shared_up, shared_down)
    dense_gate_part = jnp.dot(normal_ffn, dense_gate.T, preferred_element_type=jnp.float32)
    dense_up_part = jnp.dot(normal_ffn, dense_up.T, preferred_element_type=jnp.float32)
    dense_hidden = (jax.nn.silu(dense_gate_part) * dense_up_part).astype(jnp.bfloat16)
    dense_out = jnp.dot(dense_hidden, dense_down, preferred_element_type=jnp.float32)
    route_weight = route_scores / lax.optimization_barrier(jnp.sum(route_scores, axis=-1, keepdims=True)) * route_scale
    flat_routes = routes.reshape(-1)
    flat_weight = route_weight.reshape(-1)
    most_rows = N_EP * CAP
    slot_rank = jnp.arange(most_rows, dtype=jnp.int32)

    def one_expert(running, expert_id):
        hits = flat_routes == expert_id
        hit_count = jnp.sum(hits.astype(jnp.int32))
        picked = jnp.nonzero(hits, size=most_rows, fill_value=0)[0].astype(jnp.int32)
        is_valid = slot_rank < hit_count
        row_ids = picked // TOP_K
        outputs = swiglu(normal_ffn[row_ids], expert_gate[expert_id], expert_up[expert_id], expert_down[expert_id]).astype(jnp.bfloat16)
        added = jnp.where(is_valid[:, None], outputs.astype(jnp.float32) * flat_weight[picked][:, None], 0.0)
        return (running.at[row_ids].add(added), None)
    routed, _ = lax.scan(one_expert, jnp.zeros(residual.shape, jnp.float32), jnp.arange(EXPERTS, dtype=jnp.int32))
    combined = shared_out + routed + jax.nn.sigmoid(dense_mix) * dense_out
    layer_out = (residual + normed(combined)).astype(jnp.bfloat16)
    return (layer_out, new_keys, new_values)
```

```python
import functools

import jax
import jax.numpy as jnp
from jax import lax
from jax.experimental import pallas as pl
from jax.experimental.pallas import tpu as pltpu
from jax.sharding import PartitionSpec as P

eps = 1e-06
route_scale = 2.5
rope_base = 10000.0


def normed(values):
    return values * lax.rsqrt(jnp.mean(values * values, axis=-1, keepdims=True) + eps)


def log_decay(head_count):
    return jnp.log1p(-jnp.exp2(-5.0 - jnp.arange(head_count, dtype=jnp.float32)))


def rotate(values, positions):
    half_size = values.shape[-1] // 2
    inverse = rope_base ** (-jnp.arange(half_size, dtype=jnp.float32) / half_size)
    angles = positions.astype(jnp.float32)[:, None, None] * inverse[None, None, :]
    cosine = jnp.cos(angles)
    sine_part = jnp.sin(angles)
    first_half = values[..., :half_size]
    second = values[..., half_size:]
    return jnp.concatenate(
        [first_half * cosine - second * sine_part, first_half * sine_part + second * cosine],
        axis=-1,
    )


def retain(
    tokens, lengths, mix_gain, w_query, w_key, w_value, w_out, cache_keys, cache_values, carry_state
):
    seq_count, head_count, key_size, value_size = carry_state.shape
    block_size = cache_keys.shape[1]
    widened = tokens.astype(jnp.float32)
    normal_in = (normed(widened) * mix_gain).astype(jnp.bfloat16)
    raw_query = jnp.dot(normal_in, w_query, preferred_element_type=jnp.float32).reshape(
        seq_count, head_count, key_size
    )
    raw_key = jnp.dot(normal_in, w_key, preferred_element_type=jnp.float32).reshape(
        seq_count, head_count, key_size
    )
    raw_value = jnp.dot(normal_in, w_value, preferred_element_type=jnp.float32).reshape(
        seq_count, head_count, value_size
    )
    queries = (rotate(raw_query, lengths) * key_size ** (-0.5)).astype(jnp.bfloat16)
    new_keys = rotate(raw_key, lengths).astype(jnp.bfloat16)
    new_values = raw_value.astype(jnp.bfloat16)
    filled = lengths % block_size
    decay_rate = log_decay(head_count)
    places = jnp.arange(block_size, dtype=jnp.int32)
    stored_keys = cache_keys.reshape(seq_count, block_size, head_count, key_size)
    stored_values = cache_values.reshape(seq_count, block_size, head_count, value_size)
    scores = jnp.einsum("shd,sjhd->shj", queries, stored_keys, preferred_element_type=jnp.float32)
    distance = jnp.maximum(filled[:, None] - places[None, :], 0).astype(jnp.float32)
    live_mask = places[None, :] < filled[:, None]
    weighted = jnp.where(
        live_mask[:, None, :],
        scores * jnp.exp(distance[:, None, :] * decay_rate[None, :, None]),
        0.0,
    ).astype(jnp.bfloat16)
    own_weight = jnp.sum(
        queries.astype(jnp.float32) * new_keys.astype(jnp.float32), axis=-1
    ).astype(jnp.bfloat16)
    inside = jnp.einsum(
        "shj,sjhe->she", weighted, stored_values, preferred_element_type=jnp.float32
    )
    inside = inside + own_weight.astype(jnp.float32)[:, :, None] * new_values.astype(jnp.float32)
    carried = jnp.einsum(
        "shd,shde->she", queries.astype(jnp.float32), carry_state, precision=lax.Precision.HIGHEST
    )
    carried = (
        carried
        * jnp.exp((filled.astype(jnp.float32)[:, None] + 1.0) * decay_rate[None, :])[:, :, None]
    )
    headed = (
        normed(inside + carried).astype(jnp.bfloat16).reshape(seq_count, head_count * value_size)
    )
    mixer_out = jnp.dot(headed, w_out, preferred_element_type=jnp.float32)
    residual = widened + normed(mixer_out)
    return (
        residual,
        new_keys.reshape(seq_count, head_count * key_size),
        new_values.reshape(seq_count, head_count * value_size),
    )


MESH = pl.DeviceIdType.MESH


def grid_of(count):
    cores = 2 if count % 2 == 0 else 1
    chips = count // cores
    x_size = max(d for d in range(1, chips + 1) if chips % d == 0 and d**3 <= chips)
    plane = chips // x_size
    y_size = max(d for d in range(1, plane + 1) if plane % d == 0 and d**2 <= plane)
    return plane // y_size, y_size, x_size, cores


def silu(values):
    return values * (1.0 / (1.0 + jnp.exp(-values)))


def dot(left, right):
    return jnp.dot(left, right, preferred_element_type=jnp.float32)


def dot_rows(left, right):
    return lax.dot_general(
        left, right, (((1,), (1,)), ((), ())), preferred_element_type=jnp.float32
    )


def slot_tables(routes, scores, experts):
    seq_count, top = routes.shape
    bf16 = jnp.bfloat16
    weight = scores / jnp.sum(scores, axis=-1, keepdims=True) * route_scale
    lanes = lax.broadcasted_iota(jnp.int32, (seq_count, experts), 1)
    member = jnp.zeros((seq_count, experts), jnp.float32)
    by_expert = jnp.zeros((seq_count, experts), jnp.float32)
    for k in range(top):
        named = routes[:, k : k + 1] == lanes
        member = jnp.where(named, 1.0, member)
        by_expert = jnp.where(named, weight[:, k : k + 1], by_expert)
    row = lax.broadcasted_iota(jnp.int32, (seq_count, seq_count), 0)
    column = lax.broadcasted_iota(jnp.int32, (seq_count, seq_count), 1)
    before = jnp.where(column < row, 1.0, 0.0).astype(bf16)
    rank = dot(before, member.astype(bf16))
    first = jnp.where(rank < 0.5, member, 0.0)
    second = member - first
    source = lax.broadcasted_iota(jnp.int32, (experts, 2 * experts), 0)
    slot = lax.broadcasted_iota(jnp.int32, (experts, 2 * experts), 1)
    to_first = jnp.where(slot == 2 * source, 1.0, 0.0).astype(bf16)
    to_second = jnp.where(slot == 2 * source + 1, 1.0, 0.0).astype(bf16)

    def spread(values):
        return dot((first * values).astype(bf16), to_first) + dot(
            (second * values).astype(bf16), to_second
        )

    coarse = by_expert.astype(bf16).astype(jnp.float32)
    fine = by_expert - coarse
    pick = spread(jnp.ones_like(by_expert))
    return pick.T.astype(bf16), spread(coarse).astype(bf16), spread(fine).astype(bf16)


def ffn_kernel(
    dims,
    features_ref,
    residual_ref,
    routes_ref,
    scores_ref,
    mix_ref,
    dense_gate_ref,
    dense_up_ref,
    dense_down_ref,
    expert_gate_ref,
    expert_up_ref,
    expert_down_ref,
    shared_gate_ref,
    shared_up_ref,
    shared_down_ref,
    out_ref,
    expert_gate,
    expert_up,
    expert_down,
    shared_gate,
    shared_up,
    shared_down,
    dense_weights,
    rows_out,
    rows_in,
    answers_out,
    answers_in,
    measure,
    group_tokens,
    group_part,
    in_1a,
    in_1b,
    sum_1a,
    sum_1b,
    in_2a,
    in_2b,
    local_sem,
    link_send,
    link_recv,
    row_send,
    row_recv,
):
    nz, ny, nx, nc = dims
    count = nz * ny * nx * nc
    seq_count, model = features_ref.shape
    part = model // 2
    bf16 = jnp.bfloat16
    me = lax.axis_index("ep")
    c = lax.rem(me, nc)
    x = lax.rem(me // nc, nx)
    y = lax.rem(me // (nc * nx), ny)
    z = me // (nc * nx * ny)

    def at(z_at, y_at, x_at, c_at):
        return ((z_at * ny + y_at) * nx + x_at) * nc + c_at

    barrier = pltpu.get_barrier_semaphore()

    def greet(i, carry):
        pl.semaphore_signal(
            barrier, inc=1, device_id=(lax.rem(me + i, count),), device_id_type=MESH
        )
        return carry

    lax.fori_loop(1, count, greet, 0)

    loads = [
        pltpu.make_async_copy(dense_gate_ref, dense_weights.at[0, z, c], local_sem.at[0]),
        pltpu.make_async_copy(dense_up_ref, dense_weights.at[1, z, c], local_sem.at[1]),
        pltpu.make_async_copy(dense_down_ref, dense_weights.at[2, z, c], local_sem.at[2]),
        pltpu.make_async_copy(shared_gate_ref, shared_gate, local_sem.at[3]),
        pltpu.make_async_copy(shared_up_ref, shared_up, local_sem.at[4]),
        pltpu.make_async_copy(shared_down_ref, shared_down, local_sem.at[5]),
        pltpu.make_async_copy(expert_gate_ref.at[0], expert_gate, local_sem.at[6]),
        pltpu.make_async_copy(expert_up_ref.at[0], expert_up, local_sem.at[7]),
        pltpu.make_async_copy(expert_down_ref.at[0], expert_down, local_sem.at[8]),
    ]
    for load in loads:
        load.start()

    y_peers = [lax.rem(y + d, ny) for d in range(1, ny)]
    x_peers = [lax.rem(x + d, nx) for d in range(1, nx)]
    z_ids = [at(lax.rem(z + d, nz), y, x, c) for d in range(1, nz)]
    y_ids = [at(z, p, x, c) for p in y_peers]
    x_ids = [at(z, y, p, c) for p in x_peers]
    core_id = at(z, y, x, nc - 1 - c)

    slots = iter(range(1000))
    sent = []

    def copy(src, dst, peer):
        slot = next(slots)
        made = pltpu.make_async_remote_copy(
            src_ref=src,
            dst_ref=dst,
            send_sem=link_send.at[slot],
            recv_sem=link_recv.at[slot],
            device_id=(peer,),
            device_id_type=MESH,
        )
        made.start()
        sent.append(made)
        return made

    def arrive(copies):
        for made in copies:
            made.wait_recv()

    def pair_of(ref, device):
        return ref.at[pl.ds(pl.multiple_of(2 * device, 2), 2), :]

    def exchange(source, target, phase):
        def send(i, carry):
            peer = lax.rem(me + i, count)
            pltpu.make_async_remote_copy(
                src_ref=pair_of(source, peer),
                dst_ref=pair_of(target, me),
                send_sem=row_send.at[phase],
                recv_sem=row_recv.at[phase],
                device_id=(peer,),
                device_id_type=MESH,
            ).start()
            return carry

        lax.fori_loop(1, count, send, 0)

    def everything(phase):
        return pltpu.make_async_remote_copy(
            src_ref=measure,
            dst_ref=measure,
            send_sem=row_send.at[phase],
            recv_sem=row_recv.at[phase],
            device_id=(core_id,),
            device_id_type=MESH,
        )

    row = lax.broadcasted_iota(jnp.int32, rows_in.shape, 0)
    mine = (row >= 2 * me) & (row < 2 * me + 2)

    def completed(own, received):
        return jnp.where(mine, own[...].astype(jnp.float32), received[...].astype(jnp.float32))

    pick, coarse, fine = slot_tables(routes_ref[...], scores_ref[...], count)
    features = features_ref[...]
    group_tokens[y, x] = features
    rows_out[...] = dot(pick, features).astype(bf16)
    for load in loads[:3]:
        load.wait()

    pl.semaphore_wait(barrier, count - 1)

    first, last = pl.ds(0, part), pl.ds(part, part)
    gather_1a = []
    gather_1b = []
    view = group_tokens.at[y, x, :, first]
    gather_1a += [copy(view, view, p) for p in x_ids]
    view = group_tokens.at[y, x, :, last]
    gather_1b += [copy(view, view, p) for p in y_ids]
    exchange(rows_out, rows_in, 0)
    view = dense_weights.at[:, z, c]
    from_z = [copy(view, view, p) for p in z_ids]
    for load in loads[3:6]:
        load.wait()
    shared_hidden = (silu(dot(features, shared_gate[...])) * dot(features, shared_up[...])).astype(
        bf16
    )
    shared_out = dot(shared_hidden, shared_down[...])
    arrive(gather_1a)
    view = group_tokens.at[y, :, :, first]
    gather_2 = [copy(view, view, p) for p in y_ids]
    arrive(gather_1b)
    view = group_tokens.at[:, x, :, last]
    gather_2 += [copy(view, view, p) for p in x_ids]
    arrive(from_z)
    view = dense_weights.at[:, :, c]
    from_core = [copy(view, view, core_id)]

    for load in loads[6:]:
        load.wait()
    everything(0).wait_recv()
    inputs = completed(rows_out, rows_in).astype(bf16)
    hidden = (silu(dot(inputs, expert_gate[...])) * dot(inputs, expert_up[...])).astype(bf16)
    answers_out[...] = dot(hidden, expert_down[...]).astype(bf16)
    exchange(answers_out, answers_in, 1)

    arrive(gather_2)
    arrive(from_core)
    units = nz * nc * dense_gate_ref.shape[0]
    inputs = group_tokens[...].reshape(ny * nx * seq_count, model)
    hidden = (
        silu(dot_rows(inputs, dense_weights[0].reshape(units, model)))
        * dot_rows(inputs, dense_weights[1].reshape(units, model))
    ).astype(bf16)
    group_part[...] = (
        dot(hidden, dense_weights[2].reshape(units, model))
        .astype(bf16)
        .reshape(ny, nx, seq_count, model)
    )
    step = []
    for d, (p, peer) in enumerate(zip(y_peers, y_ids)):
        step.append(copy(group_part.at[p, :, :, first], in_1a.at[d], peer))
    for d, (p, peer) in enumerate(zip(x_peers, x_ids)):
        step.append(copy(group_part.at[:, p, :, last], in_1b.at[d], peer))

    def add(*terms):
        total = terms[0].astype(jnp.float32)
        for term in terms[1:]:
            total = total + term.astype(jnp.float32)
        return total

    arrive(step)
    sum_1a[...] = add(group_part[y, :, :, :part], *[in_1a[d] for d in range(ny - 1)]).astype(bf16)
    sum_1b[...] = add(group_part[:, x, :, part:], *[in_1b[d] for d in range(nx - 1)]).astype(bf16)
    step = []
    for d, (p, peer) in enumerate(zip(x_peers, x_ids)):
        step.append(copy(sum_1a.at[p], in_2a.at[d], peer))
    for d, (p, peer) in enumerate(zip(y_peers, y_ids)):
        step.append(copy(sum_1b.at[p], in_2b.at[d], peer))
    arrive(step)
    dense_out = jnp.concatenate(
        [
            add(sum_1a[x], *[in_2a[d] for d in range(nx - 1)]),
            add(sum_1b[y], *[in_2b[d] for d in range(ny - 1)]),
        ],
        axis=-1,
    )
    gate = 1.0 / (1.0 + jnp.exp(-mix_ref[...]))
    combined = shared_out + gate * dense_out

    everything(1).wait_recv()
    answers = completed(answers_out, answers_in).astype(bf16)
    combined = combined + (dot(coarse, answers) + dot(fine, answers))
    out_ref[...] = (residual_ref[...] + normed(combined)).astype(bf16)
    for made in sent + [everything(0), everything(1)]:
        made.wait_send()


def ffn(features, residual, routes, scores, mix, weights):
    dims = grid_of(lax.axis_size("ep"))
    nz, ny, nx, nc = dims
    count = lax.axis_size("ep")
    seq_count, model = features.shape
    part = model // 2
    bf16 = jnp.bfloat16
    dense_gate, expert_gate, expert_down, shared_gate, shared_down = (
        weights[0],
        weights[3],
        weights[5],
        weights[6],
        weights[8],
    )
    copies = 4 * (ny - 1) + 4 * (nx - 1) + (nz - 1) + 1

    def room(*shape):
        return pltpu.VMEM(shape, bf16)

    rows = (2 * count, model)
    scratch = [
        room(*expert_gate.shape[1:]),
        room(*expert_gate.shape[1:]),
        room(*expert_down.shape[1:]),
        room(*shared_gate.shape),
        room(*shared_gate.shape),
        room(*shared_down.shape),
        room(3, nz, nc, *dense_gate.shape),
        room(*rows),
        room(*rows),
        room(*rows),
        room(*rows),
        room(2 * (count - 1) * model // 256, 256),
        room(ny, nx, seq_count, model),
        room(ny, nx, seq_count, model),
        room(ny - 1, nx, seq_count, part),
        room(nx - 1, ny, seq_count, part),
        room(nx, seq_count, part),
        room(ny, seq_count, part),
        room(nx - 1, seq_count, part),
        room(ny - 1, seq_count, part),
        pltpu.SemaphoreType.DMA((9,)),
        pltpu.SemaphoreType.DMA((copies,)),
        pltpu.SemaphoreType.DMA((copies,)),
        pltpu.SemaphoreType.DMA((2,)),
        pltpu.SemaphoreType.DMA((2,)),
    ]
    vmem = pl.BlockSpec(memory_space=pltpu.VMEM)
    return pl.pallas_call(
        functools.partial(ffn_kernel, dims),
        out_shape=jax.ShapeDtypeStruct((seq_count, model), bf16),
        in_specs=[vmem] * 5 + [pl.BlockSpec(memory_space=pl.ANY)] * len(weights),
        out_specs=vmem,
        scratch_shapes=scratch,
        compiler_params=pltpu.CompilerParams(
            collective_id=0, has_side_effects=True, vmem_limit_bytes=56 * 2**20
        ),
    )(features, residual, routes, scores, mix, *weights)


def per_device(
    tokens,
    lengths,
    cache_keys,
    cache_values,
    retention_state,
    mix_gain,
    query_weight,
    key_weight,
    value_weight,
    out_weight,
    ffn_gain,
    routes,
    route_scores,
    expert_gate,
    expert_up,
    expert_down,
    shared_gate,
    shared_up,
    shared_down,
    dense_gate,
    dense_up,
    dense_down,
    dense_mix,
):
    residual, new_keys, new_values = retain(
        tokens,
        lengths,
        mix_gain,
        query_weight,
        key_weight,
        value_weight,
        out_weight,
        cache_keys,
        cache_values,
        retention_state,
    )
    features = (normed(residual) * ffn_gain).astype(jnp.bfloat16)
    weights = (
        dense_gate,
        dense_up,
        dense_down,
        expert_gate,
        expert_up,
        expert_down,
        shared_gate,
        shared_up,
        shared_down,
    )
    layer_out = ffn(features, residual, routes, route_scores, dense_mix[None, :], weights)
    return (layer_out, new_keys, new_values)


def solution(mesh):
    in_specs = (
        P("ep", None),
        P("ep"),
        P("ep", None, None),
        P("ep", None, None),
        P("ep", None, None, None),
        P(),
        P(),
        P(),
        P(),
        P(),
        P(),
        P("ep", None),
        P("ep", None),
        P("ep", None, None),
        P("ep", None, None),
        P("ep", None, None),
        P(),
        P(),
        P(),
        P("ep", None),
        P("ep", None),
        P("ep", None),
        P(),
    )
    out_specs = (P("ep", None), P("ep", None), P("ep", None))
    return jax.shard_map(
        per_device, mesh=mesh, in_specs=in_specs, out_specs=out_specs, check_vma=False
    )
```

```python
import functools
import math

import jax
import jax.numpy as jnp
from jax import lax
from jax.experimental import pallas as pl
from jax.experimental.pallas import tpu as pltpu
from jax.sharding import PartitionSpec as P

eps = 1e-06
route_scale = 2.5
rope_base = 10000.0


def normed(values):
    return values * lax.rsqrt(jnp.mean(values * values, axis=-1, keepdims=True) + eps)


MESH = pl.DeviceIdType.MESH


def grid_of(count):
    cores = 2 if count % 2 == 0 else 1
    chips = count // cores
    x_size = max(d for d in range(1, chips + 1) if chips % d == 0 and d**3 <= chips)
    plane = chips // x_size
    y_size = max(d for d in range(1, plane + 1) if plane % d == 0 and d**2 <= plane)
    return plane // y_size, y_size, x_size, cores


def silu(values):
    return values * (1.0 / (1.0 + jnp.exp(-values)))


def dot(left, right):
    return jnp.dot(left, right, preferred_element_type=jnp.float32)


def dot_rows(left, right):
    return lax.dot_general(
        left, right, (((1,), (1,)), ((), ())), preferred_element_type=jnp.float32
    )


def slot_tables(routes, scores, experts):
    top, seq_count = routes.shape
    bf16 = jnp.bfloat16
    weight = scores / jnp.sum(scores, axis=0, keepdims=True) * route_scale
    expert = lax.broadcasted_iota(jnp.int32, (experts, seq_count), 0)
    member = jnp.zeros((experts, seq_count), jnp.float32)
    by_expert = jnp.zeros((experts, seq_count), jnp.float32)
    for k in range(top):
        named = routes[k : k + 1, :] == expert
        member = jnp.where(named, 1.0, member)
        by_expert = jnp.where(named, weight[k : k + 1, :], by_expert)
    row = lax.broadcasted_iota(jnp.int32, (seq_count, seq_count), 0)
    column = lax.broadcasted_iota(jnp.int32, (seq_count, seq_count), 1)
    before = jnp.where(row < column, 1.0, 0.0).astype(bf16)
    rank = dot(member.astype(bf16), before)
    first = jnp.where(rank < 0.5, member, 0.0)
    second = member - first
    slot = lax.broadcasted_iota(jnp.int32, (2 * experts, experts), 0)
    source = lax.broadcasted_iota(jnp.int32, (2 * experts, experts), 1)
    to_first = jnp.where(slot == 2 * source, 1.0, 0.0).astype(bf16)
    to_second = jnp.where(slot == 2 * source + 1, 1.0, 0.0).astype(bf16)

    def spread(values):
        return dot(to_first, (first * values).astype(bf16)) + dot(
            to_second, (second * values).astype(bf16)
        )

    coarse = by_expert.astype(bf16).astype(jnp.float32)
    fine = by_expert - coarse
    pick = spread(jnp.ones_like(by_expert)).astype(bf16)
    return pick, spread(coarse).T.astype(bf16), spread(fine).T.astype(bf16)


def layer_kernel(
    dims,
    lengths_ref,
    tokens_hbm,
    cache_keys_hbm,
    cache_values_hbm,
    state_hbm,
    mix_gain_hbm,
    query_weight_hbm,
    key_weight_hbm,
    value_weight_hbm,
    out_weight_hbm,
    ffn_gain_hbm,
    routes_hbm,
    scores_hbm,
    expert_gate_hbm,
    expert_up_hbm,
    expert_down_hbm,
    shared_gate_hbm,
    shared_up_hbm,
    shared_down_hbm,
    dense_gate_hbm,
    dense_up_hbm,
    dense_down_hbm,
    mix_hbm,
    out_ref,
    new_keys_ref,
    new_values_ref,
    tokens,
    cache_keys,
    cache_values,
    state,
    mix_gain,
    query_weight,
    key_weight,
    value_weight,
    out_weight,
    ffn_gain,
    routes,
    scores,
    mix,
    expert_gate,
    expert_up,
    expert_down,
    shared_gate,
    shared_up,
    shared_down,
    dense_weights,
    queries,
    turned,
    block_scores,
    inside,
    carried,
    rows_out,
    rows_in,
    answers_out,
    answers_in,
    measure,
    group_tokens,
    group_part,
    in_1a,
    in_1b,
    sum_1a,
    sum_1b,
    in_2a,
    in_2b,
    local_sem,
    link_send,
    link_recv,
    row_send,
    row_recv,
    entry_sem,
):
    nz, ny, nx, nc = dims
    count = nz * ny * nx * nc
    seq_count, model = tokens.shape
    heads, key_size, value_size = state.shape[1:]
    block = cache_keys.shape[1]
    part = model // 2
    bf16 = jnp.bfloat16
    f32 = jnp.float32
    me = lax.axis_index("ep")
    c = lax.rem(me, nc)
    x = lax.rem(me // nc, nx)
    y = lax.rem(me // (nc * nx), ny)
    z = me // (nc * nx * ny)

    def at(z_at, y_at, x_at, c_at):
        return ((z_at * ny + y_at) * nx + x_at) * nc + c_at

    local_slots = iter(range(1000))

    def load(source, target):
        made = pltpu.make_async_copy(source, target, local_sem.at[next(local_slots)])
        made.start()
        return made

    def ready(loads):
        for made in loads:
            made.wait()

    chunk = seq_count // 4
    chunks = [pl.ds(i, chunk) for i in range(0, seq_count, chunk)]
    dense_loads = [
        load(dense_gate_hbm, dense_weights.at[0, z, c]),
        load(dense_up_hbm, dense_weights.at[1, z, c]),
        load(dense_down_hbm, dense_weights.at[2, z, c]),
    ]
    first_loads = [
        load(tokens_hbm, tokens),
        load(mix_gain_hbm, mix_gain),
        load(query_weight_hbm, query_weight),
        load(key_weight_hbm, key_weight),
    ]
    route_loads = [load(routes_hbm, routes), load(scores_hbm, scores)]
    key_loads = [load(cache_keys_hbm.at[s], cache_keys.at[s]) for s in chunks]
    value_loads = [load(value_weight_hbm, value_weight)]

    barrier = pltpu.get_barrier_semaphore()

    y_peers = [lax.rem(y + d, ny) for d in range(1, ny)]
    x_peers = [lax.rem(x + d, nx) for d in range(1, nx)]
    z_ids = [at(lax.rem(z + d, nz), y, x, c) for d in range(1, nz)]
    y_ids = [at(z, p, x, c) for p in y_peers]
    x_ids = [at(z, y, p, c) for p in x_peers]
    core_id = at(z, y, x, nc - 1 - c)

    across = [at(z, y, p, nc - 1 - c) for p in x_peers]
    lines = x_ids + across + [core_id] + y_ids + z_ids
    for peer in lines:
        pl.semaphore_signal(barrier, inc=1, device_id=(peer,), device_id_type=MESH)

    def spread_entry(semaphore, peers):
        for peer in peers:
            pl.semaphore_signal(semaphore, inc=1, device_id=(peer,), device_id_type=MESH)

    slots = iter(range(1000))
    sent = []

    def copy(src, dst, peer):
        slot = next(slots)
        made = pltpu.make_async_remote_copy(
            src_ref=src,
            dst_ref=dst,
            send_sem=link_send.at[slot],
            recv_sem=link_recv.at[slot],
            device_id=(peer,),
            device_id_type=MESH,
        )
        made.start()
        sent.append(made)
        return made

    def arrive(copies):
        for made in copies:
            made.wait_recv()

    def pair_of(ref, device):
        return ref.at[pl.ds(pl.multiple_of(2 * device, 2), 2), :]

    def exchange(source, target, phase):
        def send(i, carry):
            peer = lax.rem(me + i, count)
            pltpu.make_async_remote_copy(
                src_ref=pair_of(source, peer),
                dst_ref=pair_of(target, me),
                send_sem=row_send.at[phase],
                recv_sem=row_recv.at[phase],
                device_id=(peer,),
                device_id_type=MESH,
            ).start()
            return carry

        lax.fori_loop(1, count, send, 0)

    def everything(phase):
        return pltpu.make_async_remote_copy(
            src_ref=measure,
            dst_ref=measure,
            send_sem=row_send.at[phase],
            recv_sem=row_recv.at[phase],
            device_id=(core_id,),
            device_id_type=MESH,
        )

    near = pl.ds(pl.multiple_of(me // 8 * 16, 16), 16)
    near_row = lax.broadcasted_iota(jnp.int32, (16, model), 0)
    own_row = 2 * lax.rem(me, 8)
    mine = (near_row >= own_row) & (near_row < own_row + 2)

    def complete(own, received):
        received[near, :] = jnp.where(
            mine, own[near, :].astype(f32), received[near, :].astype(f32)
        ).astype(bf16)

    ready(first_loads)
    cache_loads = [load(cache_values_hbm.at[s], cache_values.at[s]) for s in chunks]
    widened = tokens[...].astype(f32)
    normal_in = (normed(widened) * mix_gain[...]).astype(bf16)
    seq_row = lax.broadcasted_iota(jnp.int32, (seq_count, 128), 0)
    length = jnp.zeros((seq_count, 128), jnp.int32)
    for s in range(seq_count):
        length = jnp.where(seq_row == s, lengths_ref[s], length)
    lane = lax.broadcasted_iota(jnp.int32, (seq_count, key_size), 1)
    half_size = key_size // 2
    turn = lax.broadcasted_iota(jnp.int32, (1, key_size), 1) % half_size
    inverse = jnp.ones((1, key_size), f32)
    for i in range(1, half_size):
        inverse = jnp.where(turn == i, rope_base ** (-i / half_size), inverse)
    angles = length.astype(f32) * inverse
    cosine = jnp.cos(angles)
    sine = jnp.where(lane < key_size // 2, -1.0, 1.0) * jnp.sin(angles)
    filled_rows = lax.rem(length, block).astype(f32)

    def rotate(values):
        pieces = []
        for h in range(heads):
            piece = values[:, h * key_size : (h + 1) * key_size]
            pieces.append(piece * cosine + pltpu.roll(piece, key_size // 2, 1) * sine)
        return jnp.concatenate(pieces, axis=-1)

    raw_query = dot(normal_in, query_weight[...])
    raw_key = dot(normal_in, key_weight[...])
    query = (rotate(raw_query) * key_size ** (-0.5)).astype(bf16).astype(f32)
    new_key = rotate(raw_key).astype(bf16)
    new_keys_ref[...] = new_key
    queries[...] = query
    turned[...] = query.T
    new_key = new_key.astype(f32)
    own_weight = [
        jnp.sum(
            query[:, h * key_size : (h + 1) * key_size]
            * new_key[:, h * key_size : (h + 1) * key_size],
            axis=-1,
            keepdims=True,
        )
        .astype(bf16)
        .astype(f32)
        for h in range(heads)
    ]

    ready(dense_loads)
    pl.semaphore_wait(barrier, len(lines))
    spread_entry(entry_sem.at[0], y_ids)
    view = dense_weights.at[:, z, c]
    from_z = [copy(view, view, p) for p in z_ids]

    rates = [math.log1p(-(2.0 ** (-5 - h))) for h in range(heads)]
    head_row = lax.broadcasted_iota(jnp.int32, (8, heads * key_size), 0)
    head_lane = lax.broadcasted_iota(jnp.int32, (8, heads * key_size), 1)
    place_row = lax.broadcasted_iota(jnp.int32, (8, block), 0)
    place = lax.broadcasted_iota(jnp.int32, (8, block), 1)
    rate = jnp.zeros((8, block), f32)
    for h in range(heads):
        rate = jnp.where(place_row == h, rates[h], rate)
    of_head = head_lane // key_size == head_row
    state_loads = []
    for i, made in enumerate(key_loads):
        made.wait()
        state_loads.append(load(state_hbm.at[chunks[i]], state.at[chunks[i]]))
        for s in range(i * chunk, (i + 1) * chunk):
            spread = jnp.where(of_head, queries[s : s + 1, :], 0.0).astype(bf16)
            found = dot_rows(spread, cache_keys[s])
            filled = lax.rem(lengths_ref[s], block)
            distance = jnp.maximum(filled - place, 0).astype(f32)
            block_scores[s] = jnp.where(
                place < filled, found * jnp.exp(distance * rate), 0.0
            ).astype(bf16)

    pl.semaphore_wait(entry_sem.at[0], len(y_ids))
    spread_entry(entry_sem.at[1], z_ids)
    ready(value_loads)
    out_loads = [load(out_weight_hbm, out_weight), load(ffn_gain_hbm, ffn_gain)]
    new_value = dot(normal_in, value_weight[...]).astype(bf16)
    new_values_ref[...] = new_value

    value_row = lax.broadcasted_iota(jnp.int32, (8, model), 0)
    value_lane = lax.broadcasted_iota(jnp.int32, (8, model), 1)
    of_value = value_lane // value_size == value_row
    for i, made in enumerate(cache_loads):
        made.wait()
        for s in range(i * chunk, (i + 1) * chunk):
            found = dot(block_scores[s], cache_values[s])
            inside[s : s + 1, :] = jnp.sum(
                jnp.where(of_value, found, 0.0), axis=0, keepdims=True
            )

    expert_loads = [
        load(expert_gate_hbm.at[0], expert_gate),
        load(expert_up_hbm.at[0], expert_up),
        load(expert_down_hbm.at[0], expert_down),
        load(mix_hbm, mix),
    ]
    shared_loads = [
        load(shared_gate_hbm, shared_gate),
        load(shared_up_hbm, shared_up),
        load(shared_down_hbm, shared_down),
    ]
    ready(route_loads)
    pick, coarse, fine = slot_tables(routes[...], scores[...], count)

    for i, made in enumerate(state_loads):
        made.wait()
        for s in range(i * chunk, (i + 1) * chunk):
            for h in range(heads):
                weights = turned[h * key_size : (h + 1) * key_size, s : s + 1]
                carried[s : s + 1, h * value_size : (h + 1) * value_size] = jnp.sum(
                    state[s, h] * weights, axis=0, keepdims=True
                )

    headed = []
    for h in range(heads):
        span = slice(h * value_size, (h + 1) * value_size)
        decay = jnp.exp((filled_rows[:, :1] + 1.0) * rates[h])
        retained = (
            inside[:, span]
            + own_weight[h] * new_value[:, span].astype(f32)
            + decay * carried[:, span]
        )
        headed.append(normed(retained).astype(bf16))
    ready(out_loads)
    mixer_out = dot(jnp.concatenate(headed, axis=-1), out_weight[...])
    residual = widened + normed(mixer_out)
    features = (normed(residual) * ffn_gain[...]).astype(bf16)

    pl.semaphore_wait(entry_sem.at[1], len(z_ids))
    group_tokens[y, x] = features
    rows_out[...] = dot(pick, features).astype(bf16)

    first, last = pl.ds(0, part), pl.ds(part, part)
    view = group_tokens.at[y, x, :, first]
    gather_1a = [copy(view, view, p) for p in x_ids]
    view = group_tokens.at[y, x, :, last]
    gather_1b = [copy(view, view, p) for p in y_ids]
    exchange(rows_out, rows_in, 0)
    ready(shared_loads)
    shared_hidden = (silu(dot(features, shared_gate[...])) * dot(features, shared_up[...])).astype(
        bf16
    )
    shared_out = dot(shared_hidden, shared_down[...])
    arrive(from_z)
    view = dense_weights.at[:, :, c]
    from_core = [copy(view, view, core_id)]
    arrive(gather_1a)
    view = group_tokens.at[y, :, :, first]
    gather_2 = [copy(view, view, p) for p in y_ids]
    arrive(gather_1b)
    view = group_tokens.at[:, x, :, last]
    gather_2 += [copy(view, view, p) for p in x_ids]

    ready(expert_loads)
    everything(0).wait_recv()
    complete(rows_out, rows_in)
    inputs = rows_in[...]
    hidden = (silu(dot(inputs, expert_gate[...])) * dot(inputs, expert_up[...])).astype(bf16)
    answers_out[...] = dot(hidden, expert_down[...]).astype(bf16)
    exchange(answers_out, answers_in, 1)

    arrive(gather_2)
    arrive(from_core)
    units = nz * nc * dense_gate_hbm.shape[0]
    inputs = group_tokens[...].reshape(ny * nx * seq_count, model)
    hidden = (
        silu(dot_rows(inputs, dense_weights[0].reshape(units, model)))
        * dot_rows(inputs, dense_weights[1].reshape(units, model))
    ).astype(bf16)
    group_part[...] = (
        dot(hidden, dense_weights[2].reshape(units, model))
        .astype(bf16)
        .reshape(ny, nx, seq_count, model)
    )
    step = []
    for d, (p, peer) in enumerate(zip(y_peers, y_ids)):
        step.append(copy(group_part.at[p, :, :, first], in_1a.at[d], peer))
    for d, (p, peer) in enumerate(zip(x_peers, x_ids)):
        step.append(copy(group_part.at[:, p, :, last], in_1b.at[d], peer))

    def add(*terms):
        total = terms[0].astype(f32)
        for term in terms[1:]:
            total = total + term.astype(f32)
        return total

    arrive(step)
    sum_1a[...] = add(group_part[y, :, :, :part], *[in_1a[d] for d in range(ny - 1)]).astype(bf16)
    sum_1b[...] = add(group_part[:, x, :, part:], *[in_1b[d] for d in range(nx - 1)]).astype(bf16)
    step = []
    for d, (p, peer) in enumerate(zip(x_peers, x_ids)):
        step.append(copy(sum_1a.at[p], in_2a.at[d], peer))
    for d, (p, peer) in enumerate(zip(y_peers, y_ids)):
        step.append(copy(sum_1b.at[p], in_2b.at[d], peer))
    arrive(step)
    dense_out = jnp.concatenate(
        [
            add(sum_1a[x], *[in_2a[d] for d in range(nx - 1)]),
            add(sum_1b[y], *[in_2b[d] for d in range(ny - 1)]),
        ],
        axis=-1,
    )
    gate = 1.0 / (1.0 + jnp.exp(-mix[...]))
    combined = shared_out + gate * dense_out

    everything(1).wait_recv()
    complete(answers_out, answers_in)
    answers = answers_in[...]
    combined = combined + (dot(coarse, answers) + dot(fine, answers))
    out_ref[...] = (residual + normed(combined)).astype(bf16)
    for made in sent + [everything(0), everything(1)]:
        made.wait_send()


def hand_over(a_ref, b_ref, c_ref, a_out, b_out, c_out, sems):
    pairs = ((a_ref, a_out), (b_ref, b_out), (c_ref, c_out))
    moves = [pltpu.make_async_copy(*pair, sems.at[i]) for i, pair in enumerate(pairs)]
    for move in moves:
        move.start()
    for move in moves:
        move.wait()


def per_device(
    tokens,
    lengths,
    cache_keys,
    cache_values,
    retention_state,
    mix_gain,
    query_weight,
    key_weight,
    value_weight,
    out_weight,
    ffn_gain,
    routes,
    route_scores,
    expert_gate,
    expert_up,
    expert_down,
    shared_gate,
    shared_up,
    shared_down,
    dense_gate,
    dense_up,
    dense_down,
    dense_mix,
):
    count = lax.axis_size("ep")
    dims = grid_of(count)
    nz, ny, nx, nc = dims
    seq_count, model = tokens.shape
    heads, key_size, value_size = retention_state.shape[1:]
    block = cache_keys.shape[1]
    part = model // 2
    bf16 = jnp.bfloat16
    f32 = jnp.float32
    operands = (
        tokens,
        cache_keys,
        cache_values,
        retention_state,
        mix_gain[None, :],
        query_weight,
        key_weight,
        value_weight,
        out_weight,
        ffn_gain[None, :],
        routes.T,
        route_scores.T,
        expert_gate,
        expert_up,
        expert_down,
        shared_gate,
        shared_up,
        shared_down,
        dense_gate,
        dense_up,
        dense_down,
        dense_mix[None, :],
    )
    copies = 4 * (ny - 1) + 4 * (nx - 1) + (nz - 1) + 1

    def room(*shape):
        return pltpu.VMEM(shape, bf16)

    def like(array):
        return pltpu.VMEM(array.shape, array.dtype)

    rows = (2 * count, model)
    scratch = [
        like(tokens),
        like(cache_keys),
        like(cache_values),
        like(retention_state),
        pltpu.VMEM((1, model), f32),
        like(query_weight),
        like(key_weight),
        like(value_weight),
        like(out_weight),
        pltpu.VMEM((1, model), f32),
        pltpu.VMEM(routes.shape[::-1], routes.dtype),
        pltpu.VMEM(route_scores.shape[::-1], f32),
        pltpu.VMEM((1, model), f32),
        room(*expert_gate.shape[1:]),
        room(*expert_gate.shape[1:]),
        room(*expert_down.shape[1:]),
        like(shared_gate),
        like(shared_up),
        like(shared_down),
        room(3, nz, nc, *dense_gate.shape),
        pltpu.VMEM((seq_count, heads * key_size), f32),
        pltpu.VMEM((heads * key_size, seq_count), f32),
        room(seq_count, 8, block),
        pltpu.VMEM((seq_count, model), f32),
        pltpu.VMEM((seq_count, model), f32),
        room(*rows),
        room(*rows),
        room(*rows),
        room(*rows),
        room(2 * (count - 1) * model // 256, 256),
        room(ny, nx, seq_count, model),
        room(ny, nx, seq_count, model),
        room(ny - 1, nx, seq_count, part),
        room(nx - 1, ny, seq_count, part),
        room(nx, seq_count, part),
        room(ny, seq_count, part),
        room(nx - 1, seq_count, part),
        room(ny - 1, seq_count, part),
        pltpu.SemaphoreType.DMA((40,)),
        pltpu.SemaphoreType.DMA((copies,)),
        pltpu.SemaphoreType.DMA((copies,)),
        pltpu.SemaphoreType.DMA((2,)),
        pltpu.SemaphoreType.DMA((2,)),
        pltpu.SemaphoreType.REGULAR((2,)),
    ]
    vmem = pl.BlockSpec(memory_space=pltpu.VMEM)
    shapes = [(seq_count, model), (seq_count, heads * key_size), (seq_count, model)]
    made = pl.pallas_call(
        functools.partial(layer_kernel, dims),
        out_shape=tuple(pltpu.VMEM(shape, bf16) for shape in shapes),
        in_specs=[pl.BlockSpec(memory_space=pltpu.SMEM)]
        + [pl.BlockSpec(memory_space=pl.ANY)] * len(operands),
        out_specs=(vmem, vmem, vmem),
        scratch_shapes=scratch,
        compiler_params=pltpu.CompilerParams(
            collective_id=0, has_side_effects=True, vmem_limit_bytes=56 * 2**20
        ),
    )(lengths, *operands)
    return tuple(
        pl.pallas_call(
            hand_over,
            out_shape=tuple(jax.ShapeDtypeStruct(shape, bf16) for shape in shapes),
            in_specs=[vmem] * 3,
            out_specs=[pl.BlockSpec(memory_space=pl.ANY)] * 3,
            scratch_shapes=[pltpu.SemaphoreType.DMA((3,))],
        )(*[pltpu.with_memory_space_constraint(m, pltpu.VMEM) for m in made])
    )


def solution(mesh):
    in_specs = (
        P("ep", None),
        P("ep"),
        P("ep", None, None),
        P("ep", None, None),
        P("ep", None, None, None),
        P(),
        P(),
        P(),
        P(),
        P(),
        P(),
        P("ep", None),
        P("ep", None),
        P("ep", None, None),
        P("ep", None, None),
        P("ep", None, None),
        P(),
        P(),
        P(),
        P("ep", None),
        P("ep", None),
        P("ep", None),
        P(),
    )
    out_specs = (P("ep", None), P("ep", None), P("ep", None))
    return jax.shard_map(
        per_device, mesh=mesh, in_specs=in_specs, out_specs=out_specs, check_vma=False
    )
```
